32 devices in a mesh: sp: 8 (over z, y), tp: 4 (over x, core).
Axes of the slice: x: 2, y: 2, z: 4, core: 2. Of those that a mesh axis runs over, the one named last changes fastest.
Arguments:
- activations: bfloat16 [6144, 2048], P(('sp', 'tp')), may hold values from -6 to 6
- in_gain: float32 [2048], replicated, may hold values from 0.1 to 1.9
- w_pool_in: bfloat16 [2048, 1024], P(None, 'tp'), may hold values from -0.125 to 0.125
- pool_gain: float32 [1024], P('tp'), may hold values from 0.1 to 1.9
- w_qlat: bfloat16 [2048, 768], P(None, 'tp'), may hold values from -0.125 to 0.125
- w_kvlat: bfloat16 [2048, 512], P(None, 'tp'), may hold values from -0.125 to 0.125
- w_krope: bfloat16 [2048, 32], replicated, may hold values from -0.125 to 0.125
- qlat_gain: float32 [768], replicated, may hold values from 0.1 to 1.9
- kvlat_gain: float32 [512], replicated, may hold values from 0.1 to 1.9
- w_qup: bfloat16 [768, 1536], P(None, 'tp'), may hold values from -0.21875 to 0.21875
- w_kup: bfloat16 [512, 1024], P(None, 'tp'), may hold values from -0.25 to 0.25
- w_vup: bfloat16 [512, 1024], P(None, 'tp'), may hold values from -0.25 to 0.25
- qhead_gain: float32 [96], replicated, may hold values from 1.1 to 1.9
- khead_gain: float32 [96], replicated, may hold values from 1.1 to 1.9
- w_out_pool: bfloat16 [1024, 2048], P('tp'), may hold values from -0.1875 to 0.1875
- w_out_attn: bfloat16 [1024, 2048], P('tp'), may hold values from -0.75 to 0.75
Outputs:
- mixed: bfloat16 [6144, 2048], P(('sp', 'tp'))
The draws below stay inside these ranges and needn't reach their ends.
All inputs are finite; a program needn't handle non-finite values.
Results may differ from the reference program's by a relative error of at most 0.025.
Values may be sent and summed in bfloat16 or wider, within the bound.
A program may use at most 128 MiB of HBM per device.

```python
import math
import jax
import jax.numpy as jnp
from jax import lax

D = 2048
POOL = 1024
GROUP = 256
HEADS = 16
NOPE = 64
ROPE = 32
VDIM = 64
QLAT = 768
KVLAT = 512
TOKENS = 6144
N_TP = 4


def level_of(stream_key, extent, split, low, top_value):
    def one(axis_at, shards_of):
        draws = jax.random.uniform(jax.random.fold_in(jax.random.fold_in(stream_key, 6), axis_at), (shards_of,), jnp.float32, low / len(split), top_value / len(split))
        return jnp.repeat(jnp.exp(draws), extent[axis_at] // shards_of).reshape((-1,) + (1,) * (len(extent) - axis_at - 1))

    level = one(*split[0])
    for cut in split[1:]:
        level = level * one(*cut)
    return level


def noise(own_key, shape, scale, reach, cuts=(), kind=jnp.bfloat16):
    array = jax.random.normal(own_key, shape, jnp.float32) * scale
    if len(cuts) > 0:
        array = level_of(own_key, shape, cuts, -0.22, 0.18) * array
    return jnp.clip(array, min=-reach, max=reach).astype(kind)


def setup_inputs(seed: int = 0) -> dict:
    streams_of = jax.random.split(jax.random.key(seed), 17)
    activations = noise(streams_of[0], (TOKENS, D), 1.0, 6.0, ((0, 32),))
    in_gain = jnp.clip(1.0 + 0.18 * jax.random.normal(streams_of[1], (D,), jnp.float32), 0.1, 1.9)
    w_pool_in = noise(streams_of[2], (D, POOL), D ** -0.5, 0.125, ((1, 4),))
    pool_gain = jnp.clip(1.0 + 0.18 * jax.random.normal(streams_of[3], (POOL,), jnp.float32), 0.1, 1.9)
    w_qlat = noise(streams_of[4], (D, QLAT), D ** -0.5, 0.125, ((1, 4),))
    w_kvlat = noise(streams_of[5], (D, KVLAT), D ** -0.5, 0.125, ((1, 4),))
    w_krope = noise(streams_of[6], (D, ROPE), D ** -0.5, 0.125)
    qlat_gain = jnp.clip(1.0 + 0.18 * jax.random.normal(streams_of[7], (QLAT,), jnp.float32), 0.1, 1.9)
    kvlat_gain = jnp.clip(1.0 + 0.18 * jax.random.normal(streams_of[8], (KVLAT,), jnp.float32), 0.1, 1.9)
    w_qup = noise(streams_of[9], (QLAT, HEADS * (NOPE + ROPE)), QLAT ** -0.5, 0.21875, ((1, 4),))
    w_kup = noise(streams_of[10], (KVLAT, HEADS * NOPE), KVLAT ** -0.5, 0.25, ((1, 4),))
    w_vup = noise(streams_of[11], (KVLAT, HEADS * VDIM), KVLAT ** -0.5, 0.25, ((1, 4),))
    qhead_gain = jnp.clip(jax.random.uniform(streams_of[12], (NOPE + ROPE,), jnp.float32, 1.1, 1.9), 1.1, 1.9)
    khead_gain = jnp.clip(jax.random.uniform(streams_of[13], (NOPE + ROPE,), jnp.float32, 1.1, 1.9), 1.1, 1.9)
    w_out_pool = noise(streams_of[14], (POOL, D), POOL ** -0.5, 0.1875, ((0, 4),))
    w_out_attn = noise(streams_of[15], (HEADS * VDIM, D), (HEADS * VDIM // 16) ** -0.5, 0.75, ((0, 4),))
    return {"activations": activations, "in_gain": in_gain, "w_pool_in": w_pool_in, "pool_gain": pool_gain, "w_qlat": w_qlat, "w_kvlat": w_kvlat, "w_krope": w_krope, "qlat_gain": qlat_gain, "kvlat_gain": kvlat_gain, "w_qup": w_qup, "w_kup": w_kup, "w_vup": w_vup, "qhead_gain": qhead_gain, "khead_gain": khead_gain, "w_out_pool": w_out_pool, "w_out_attn": w_out_attn}


norm_eps = 1e-06
rope_theta = 10000.0
rim_depth = 15
block_rows = 512

def row_norm(source, norm_gain):
    as_float = source.astype(jnp.float32)
    factor = lax.rsqrt(lax.optimization_barrier(jnp.mean(as_float * as_float, axis=-1, keepdims=True)) + norm_eps)
    return as_float * factor * norm_gain

def rotate(head_rows, positions):
    half_rope = ROPE // 2
    frequency = rope_theta ** (-jnp.arange(0, ROPE, 2, dtype=jnp.float32) / ROPE)
    angles = positions.astype(jnp.float32)[:, None] * frequency[None, :]
    cosine = jnp.cos(angles)[:, None, :]
    sine_part = jnp.sin(angles)[:, None, :]
    plain_part = head_rows[..., :NOPE]
    lower_half = head_rows[..., NOPE:NOPE + half_rope]
    upper_half = head_rows[..., NOPE + half_rope:]
    return jnp.concatenate([plain_part, lower_half * cosine - upper_half * sine_part, upper_half * cosine + lower_half * sine_part], axis=-1)

def pool_mix(extended, positions, channel_start):
    row_count = positions.shape[0]
    width = extended.shape[1]
    channel = channel_start + jnp.arange(width, dtype=jnp.int32)
    window = jnp.left_shift(jnp.int32(2), (channel // GROUP).astype(jnp.int32))
    as_float = extended.astype(jnp.float32)
    window_sum = jnp.zeros((row_count, width), jnp.float32)
    for lag_index in range(rim_depth + 1):
        lagged = as_float[rim_depth - lag_index:rim_depth - lag_index + row_count]
        window_sum = window_sum + jnp.where(lag_index < window[None, :], lagged, 0.0)
    divisor = jnp.minimum(positions[:, None] + 1, window[None, :]).astype(jnp.float32)
    return window_sum / divisor - as_float[rim_depth:]

def make_queries(q_normed, w_qup, norm_gain, positions):
    row_count = q_normed.shape[0]
    head_count = w_qup.shape[1] // (NOPE + ROPE)
    query_raw = jnp.dot(q_normed, w_qup, preferred_element_type=jnp.float32).astype(jnp.bfloat16)
    query_raw = query_raw.reshape(row_count, head_count, NOPE + ROPE)
    return rotate(row_norm(query_raw, norm_gain), positions).astype(jnp.bfloat16)

def make_keys(kv_rows, rope_rows, w_kup, w_vup, norm_gain, positions):
    row_count = kv_rows.shape[0]
    head_count = w_kup.shape[1] // NOPE
    key_plain = jnp.dot(kv_rows, w_kup, preferred_element_type=jnp.float32).astype(jnp.bfloat16)
    key_plain = key_plain.reshape(row_count, head_count, NOPE)
    value_rows = jnp.dot(kv_rows, w_vup, preferred_element_type=jnp.float32).astype(jnp.bfloat16)
    shared = jnp.broadcast_to(rope_rows[:, None, :], (row_count, head_count, ROPE))
    joined = jnp.concatenate([key_plain, shared], axis=-1)
    key_rows = rotate(row_norm(joined, norm_gain), positions).astype(jnp.bfloat16)
    return (key_rows.reshape(row_count, head_count * (NOPE + ROPE)), value_rows)

def attend(queries, key_rows, value_rows):
    all_rows, head_count, _ = queries.shape
    block_size = math.gcd(block_rows, all_rows)
    key_rows = key_rows.reshape(all_rows, head_count, NOPE + ROPE)
    value_rows = value_rows.reshape(all_rows, head_count, VDIM)
    score_scale = (NOPE + ROPE) ** (-0.5)

    def one_block(block_index):
        first_row = block_index * block_size
        query_block = lax.dynamic_slice_in_dim(queries, first_row, block_size, 0).astype(jnp.float32)
        query_pos = first_row + jnp.arange(block_size, dtype=jnp.int32)

        def add_keys(key_index, state_pair):
            numerator, denominator = state_pair
            key_first = key_index * block_size
            key_block = lax.dynamic_slice_in_dim(key_rows, key_first, block_size, 0).astype(jnp.float32)
            value_block = lax.dynamic_slice_in_dim(value_rows, key_first, block_size, 0).astype(jnp.float32)
            key_pos = key_first + jnp.arange(block_size, dtype=jnp.int32)
            scores = jnp.einsum('qhd,khd->hqk', query_block, key_block) * score_scale
            weights = jnp.where(key_pos[None, None, :] <= query_pos[None, :, None], jnp.exp(scores), 0.0)
            denominator = denominator + lax.optimization_barrier(jnp.sum(weights, axis=-1))
            rounded = lax.optimization_barrier(weights.astype(jnp.bfloat16)).astype(jnp.float32)
            numerator = numerator + jnp.einsum('hqk,khd->qhd', rounded, value_block)
            return (numerator, denominator)
        start_pair = (jnp.zeros((block_size, head_count, VDIM), jnp.float32), jnp.zeros((head_count, block_size), jnp.float32))
        numerator, denominator = lax.fori_loop(0, block_index + 1, add_keys, start_pair)
        return (numerator / jnp.transpose(denominator)[:, :, None]).astype(jnp.bfloat16)
    blocks_out = lax.map(one_block, jnp.arange(all_rows // block_size, dtype=jnp.int32))
    return blocks_out.reshape(all_rows, head_count * VDIM)

def reference(activations, in_gain, w_pool_in, pool_gain, w_qlat, w_kvlat, w_krope, qlat_gain, kvlat_gain, w_qup, w_kup, w_vup, qhead_gain, khead_gain, w_out_pool, w_out_attn):
    positions = jnp.arange(TOKENS, dtype=jnp.int32)
    normed = row_norm(activations, in_gain).astype(jnp.bfloat16)
    pool_in = jnp.dot(normed, w_pool_in, preferred_element_type=jnp.float32).astype(jnp.bfloat16)
    extended = jnp.concatenate([jnp.zeros((rim_depth, POOL), jnp.bfloat16), pool_in], axis=0)
    pool_out = (pool_mix(extended, positions, 0) * pool_gain).astype(jnp.bfloat16)
    q_latent = jnp.dot(normed, w_qlat, preferred_element_type=jnp.float32).astype(jnp.bfloat16)
    kv_latent = jnp.dot(normed, w_kvlat, preferred_element_type=jnp.float32).astype(jnp.bfloat16)
    rope_key = jnp.dot(normed, w_krope, preferred_element_type=jnp.float32).astype(jnp.bfloat16)
    q_normed = row_norm(q_latent, qlat_gain).astype(jnp.bfloat16)
    kv_normed = row_norm(kv_latent, kvlat_gain).astype(jnp.bfloat16)
    queries = make_queries(q_normed, w_qup, qhead_gain, positions)
    key_rows, value_rows = make_keys(kv_normed, rope_key, w_kup, w_vup, khead_gain, positions)
    attended = attend(queries, key_rows, value_rows)
    pool_span = POOL // N_TP
    attn_span = HEADS * VDIM // N_TP
    mixed = jnp.zeros((TOKENS, D), jnp.float32)
    for block_index in range(N_TP):
        pool_lo = block_index * pool_span
        attn_lo = block_index * attn_span
        partial_value = jnp.dot(pool_out[:, pool_lo:pool_lo + pool_span], w_out_pool[pool_lo:pool_lo + pool_span], preferred_element_type=jnp.float32)
        partial_value = partial_value + jnp.dot(attended[:, attn_lo:attn_lo + attn_span], w_out_attn[attn_lo:attn_lo + attn_span], preferred_element_type=jnp.float32)
        rounded = lax.optimization_barrier(partial_value.astype(jnp.bfloat16)).astype(jnp.float32)
        mixed = mixed + rounded
    return mixed.astype(jnp.bfloat16)
```

```python
import functools
import math

import jax
import jax.numpy as jnp
from jax import lax
from jax.experimental import pallas as pl
from jax.experimental.pallas import tpu as pltpu
from jax.sharding import PartitionSpec as P

GROUP = 256
NOPE = 64
ROPE = 32
VDIM = 64
HEAD = NOPE + ROPE
LANES = 128

norm_eps = 1e-06
rope_theta = 10000.0
rim_depth = 15
bf16 = jnp.bfloat16
f32 = jnp.float32


def from_behind(block, axis, distance):
    devices = range(lax.axis_size(axis))
    route = [(i - distance, i) for i in devices if i - distance in devices]
    return lax.ppermute(block, axis, route)


def row_norm(source, norm_gain):
    as_float = source.astype(f32)
    factor = lax.rsqrt(jnp.mean(as_float * as_float, axis=-1, keepdims=True) + norm_eps)
    return as_float * factor * norm_gain


def pool_mix(extended, positions, channel_start):
    row_count = positions.shape[0]
    width = extended.shape[1]
    channel = channel_start + jnp.arange(width, dtype=jnp.int32)
    window = jnp.left_shift(jnp.int32(2), channel // GROUP)
    as_float = extended.astype(f32)
    total = as_float
    window_sum = None
    for level in range(4):
        span = 1 << level
        total = total + jnp.concatenate([jnp.zeros((span, width), f32), total[:-span]], axis=0)
        chosen = total[rim_depth:]
        if window_sum is None:
            window_sum = chosen
        else:
            window_sum = jnp.where(window[None, :] >= 2 * span, chosen, window_sum)
    divisor = jnp.minimum(positions[:, None] + 1, window[None, :]).astype(f32)
    return window_sum / divisor - as_float[rim_depth:]


def pad_heads(weight, width):
    depth = weight.shape[0]
    heads = weight.shape[1] // width
    shaped = weight.reshape(depth, heads, width)
    return jnp.pad(shaped, ((0, 0), (0, 0), (0, LANES - width))).reshape(depth, heads * LANES)


def pad_row(gain):
    return jnp.pad(gain, (0, LANES - gain.shape[0])).reshape(1, LANES)


def rope_tables(rows, blocks):
    half = ROPE // 2
    frequency = rope_theta ** (-jnp.arange(0, ROPE, 2, dtype=f32) / ROPE)

    def make(positions):
        angles = positions.astype(f32)[:, None] * frequency[None, :]
        cosine, sine = jnp.cos(angles), jnp.sin(angles)
        count = positions.shape[0]
        rest = LANES - HEAD
        cos_row = jnp.concatenate(
            [jnp.ones((count, NOPE), f32), cosine, cosine, jnp.zeros((count, rest), f32)], axis=1
        )
        sin_row = jnp.concatenate(
            [jnp.zeros((count, NOPE), f32), sine, sine, jnp.zeros((count, rest), f32)], axis=1
        )
        return cos_row, sin_row

    return make(jnp.arange(rows)) + make(jnp.arange(blocks) * rows)


def head_finish(x, gain, cosine, sin_low, sin_high):
    factor = lax.rsqrt(jnp.sum(x * x, axis=1, keepdims=True) * (1.0 / HEAD) + norm_eps)
    y = x * factor * gain
    half = ROPE // 2
    return (
        y * cosine
        + pltpu.roll(y, LANES - half, 1) * sin_low
        + pltpu.roll(y, half, 1) * sin_high
    )


def attention_kernel(
    heads,
    step_rows,
    q_ref,
    kv_ref,
    wq_ref,
    wk_ref,
    wv_ref,
    qlat_gain,
    kvlat_gain,
    qh_gain,
    kh_gain,
    cos_r,
    sin_r,
    cos_b,
    sin_b,
    out_ref,
    kv_buf,
    queries,
    keys_t,
    values,
    acc,
    sem,
):
    rows = q_ref.shape[0]
    kvlat = wk_ref.shape[0]
    mine = lax.axis_index("sp")
    lane = lax.broadcasted_iota(jnp.int32, (step_rows, LANES), 1)
    score_scale = HEAD ** (-0.5) * math.log2(math.e)

    def fetch(block, slot):
        return pltpu.make_async_copy(kv_ref.at[block], kv_buf.at[slot], sem.at[slot])

    fetch(0, 0).start()

    def angles(block, at):
        cr, sr = cos_r[at, :], sin_r[at, :]
        cb, sb = cos_b[pl.ds(block, 1), :], sin_b[pl.ds(block, 1), :]
        cosine = jnp.where(lane < NOPE, 1.0, cr * cb - sr * sb)
        sine = sr * cb + cr * sb
        low = jnp.where((lane >= NOPE) & (lane < NOPE + ROPE // 2), -sine, 0.0)
        high = jnp.where((lane >= NOPE + ROPE // 2) & (lane < HEAD), sine, 0.0)
        return cosine, low, high

    def prepare_queries(step, _):
        at = pl.ds(pl.multiple_of(step * step_rows, step_rows), step_rows)
        normed = row_norm(q_ref[at, :], qlat_gain[...]).astype(bf16)
        raw = jnp.dot(normed, wq_ref[...], preferred_element_type=f32).astype(bf16).astype(f32)
        tables = angles(mine, at)
        for h in range(heads):
            x = raw[:, h * LANES : (h + 1) * LANES]
            y = head_finish(x, qh_gain[...], *tables)
            queries[h, at, :] = (y * score_scale).astype(bf16)
        return 0

    lax.fori_loop(0, rows // step_rows, prepare_queries, 0)
    acc[...] = jnp.zeros_like(acc)

    def prepare_keys(block, slot):
        def one(step, _):
            at = pl.ds(pl.multiple_of(step * step_rows, step_rows), step_rows)
            latent = kv_buf[slot, at, :kvlat]
            shared = kv_buf[slot, at, kvlat:].astype(f32)
            normed = row_norm(latent, kvlat_gain[...]).astype(bf16)
            plain = jnp.dot(normed, wk_ref[...], preferred_element_type=f32).astype(bf16).astype(f32)
            value = jnp.dot(normed, wv_ref[...], preferred_element_type=f32)
            tables = angles(block, at)
            for h in range(heads):
                x = plain[:, h * LANES : (h + 1) * LANES] + shared
                y = head_finish(x, kh_gain[...], *tables)
                keys_t[h, :, at] = y.T.astype(bf16)
                v = jnp.where(lane == VDIM, 1.0, value[:, h * LANES : (h + 1) * LANES])
                values[h, at, :] = v.astype(bf16)
            return 0

        lax.fori_loop(0, rows // step_rows, one, 0)

    def accumulate(on_diagonal):
        def one(step, _):
            at = pl.ds(pl.multiple_of(step * step_rows, step_rows), step_rows)
            for h in range(heads):
                scores = jnp.dot(queries[h, at, :], keys_t[h], preferred_element_type=f32)
                weights = jnp.exp2(scores)
                if on_diagonal:
                    q_pos = step * step_rows + lax.broadcasted_iota(jnp.int32, scores.shape, 0)
                    k_pos = lax.broadcasted_iota(jnp.int32, scores.shape, 1)
                    weights = jnp.where(k_pos <= q_pos, weights, 0.0)
                acc[h, at, :] += jnp.dot(weights.astype(bf16), values[h], preferred_element_type=f32)
            return 0

        lax.fori_loop(0, rows // step_rows, one, 0)

    def earlier(block, _):
        slot = lax.rem(block, 2)
        fetch(block, slot).wait()
        fetch(block + 1, 1 - slot).start()
        prepare_keys(block, slot)
        accumulate(False)
        return 0

    lax.fori_loop(0, mine, earlier, 0)
    slot = lax.rem(mine, 2)
    fetch(mine, slot).wait()
    prepare_keys(mine, slot)
    accumulate(True)

    def finish(step, _):
        at = pl.ds(pl.multiple_of(step * step_rows, step_rows), step_rows)
        parts = []
        for h in range(heads):
            a = acc[h, at, :]
            parts.append(a[:, :VDIM] / a[:, VDIM : VDIM + 1])
        out_ref[at, :] = jnp.concatenate(parts, axis=1).astype(bf16)
        return 0

    lax.fori_loop(0, rows // step_rows, finish, 0)


def attention(q_lat, kv_all, wq, wk, wv, gains, tables):
    rows = q_lat.shape[0]
    heads = wq.shape[1] // LANES
    step_rows = math.gcd(rows, 256)
    vm = pl.BlockSpec(memory_space=pltpu.VMEM)
    return pl.pallas_call(
        functools.partial(attention_kernel, heads, step_rows),
        out_shape=jax.ShapeDtypeStruct((rows, heads * VDIM), bf16),
        in_specs=[vm, pl.BlockSpec(memory_space=pl.ANY)] + [vm] * 11,
        out_specs=vm,
        scratch_shapes=[
            pltpu.VMEM((2,) + kv_all.shape[1:], bf16),
            pltpu.VMEM((heads, rows, LANES), bf16),
            pltpu.VMEM((heads, LANES, rows), bf16),
            pltpu.VMEM((heads, rows, LANES), bf16),
            pltpu.VMEM((heads, rows, LANES), f32),
            pltpu.SemaphoreType.DMA((2,)),
        ],
        compiler_params=pltpu.CompilerParams(vmem_limit_bytes=48 * 1024 * 1024),
    )(q_lat, kv_all, wq, wk, wv, *gains, *tables)


def local(
    activations,
    in_gain,
    w_pool_in,
    pool_gain,
    w_qlat,
    w_kvlat,
    w_krope,
    qlat_gain,
    kvlat_gain,
    w_qup,
    w_kup,
    w_vup,
    qhead_gain,
    khead_gain,
    w_out_pool,
    w_out_attn,
):
    own_input = lax.all_gather(activations, "tp", axis=0, tiled=True)
    row_count = own_input.shape[0]
    n_sp = lax.axis_size("sp")
    positions = lax.axis_index("sp") * row_count + jnp.arange(row_count, dtype=jnp.int32)
    normed = row_norm(own_input, in_gain).astype(bf16)
    q_part = jnp.dot(normed, w_qlat, preferred_element_type=f32).astype(bf16)
    kv_part = jnp.dot(normed, w_kvlat, preferred_element_type=f32).astype(bf16)
    krope_pad = jnp.pad(w_krope, ((0, 0), (NOPE, LANES - HEAD)))
    rope_key = jnp.dot(normed, krope_pad, preferred_element_type=f32).astype(bf16)
    q_width = q_part.shape[1]
    latents = lax.all_gather(jnp.concatenate([q_part, kv_part], axis=1), "tp", axis=0, tiled=False)
    q_lat = jnp.concatenate([latents[i, :, :q_width] for i in range(latents.shape[0])], axis=1)
    kv_lat = jnp.concatenate(
        [latents[i, :, q_width:] for i in range(latents.shape[0])] + [rope_key], axis=1
    )
    kv_all = lax.all_gather(kv_lat, "sp", axis=0, tiled=False)
    pool_in = jnp.dot(normed, w_pool_in, preferred_element_type=f32).astype(bf16)
    prev_rows = from_behind(pool_in[row_count - rim_depth :], "sp", 1)
    extended = jnp.concatenate([prev_rows, pool_in], axis=0)
    channel_start = lax.axis_index("tp") * pool_in.shape[1]
    pool_out = (pool_mix(extended, positions, channel_start) * pool_gain).astype(bf16)
    attended = attention(
        q_lat,
        kv_all,
        pad_heads(w_qup, HEAD),
        pad_heads(w_kup, NOPE),
        pad_heads(w_vup, VDIM),
        (qlat_gain.reshape(1, -1), kvlat_gain.reshape(1, -1), pad_row(qhead_gain), pad_row(khead_gain)),
        rope_tables(row_count, n_sp),
    )
    term = jnp.dot(pool_out, w_out_pool, preferred_element_type=f32)
    return lax.psum_scatter(
        (term + jnp.dot(attended, w_out_attn, preferred_element_type=f32)).astype(bf16),
        "tp",
        scatter_dimension=0,
        tiled=True,
    )


def solution(mesh):
    placed = (
        P(("sp", "tp"), None),
        P(),
        P(None, "tp"),
        P("tp"),
        P(None, "tp"),
        P(None, "tp"),
        P(),
        P(),
        P(),
        P(None, "tp"),
        P(None, "tp"),
        P(None, "tp"),
        P(),
        P(),
        P("tp", None),
        P("tp", None),
    )
    return jax.shard_map(
        local, mesh=mesh, in_specs=placed, out_specs=P(("sp", "tp"), None), check_vma=False
    )
```

```python
import functools
import math

import jax
import jax.numpy as jnp
from jax import lax
from jax.experimental import pallas as pl
from jax.experimental.pallas import tpu as pltpu
from jax.sharding import PartitionSpec as P

GROUP = 256
NOPE = 64
ROPE = 32
VDIM = 64
HEAD = NOPE + ROPE
LANES = 128

norm_eps = 1e-06
rope_theta = 10000.0
rim_depth = 15
bf16 = jnp.bfloat16
f32 = jnp.float32


def from_behind(block, axis, distance):
    devices = range(lax.axis_size(axis))
    route = [(i - distance, i) for i in devices if i - distance in devices]
    return lax.ppermute(block, axis, route)


def row_norm(source, norm_gain):
    as_float = source.astype(f32)
    factor = lax.rsqrt(jnp.mean(as_float * as_float, axis=-1, keepdims=True) + norm_eps)
    return as_float * factor * norm_gain


def pool_mix(extended, positions, channel_start):
    row_count = positions.shape[0]
    width = extended.shape[1]
    channel = channel_start + jnp.arange(width, dtype=jnp.int32)
    window = jnp.left_shift(jnp.int32(2), channel // GROUP)
    as_float = extended.astype(f32)
    total = as_float
    window_sum = None
    for level in range(4):
        span = 1 << level
        total = total + jnp.concatenate([jnp.zeros((span, width), f32), total[:-span]], axis=0)
        chosen = total[rim_depth:]
        if window_sum is None:
            window_sum = chosen
        else:
            window_sum = jnp.where(window[None, :] >= 2 * span, chosen, window_sum)
    divisor = jnp.minimum(positions[:, None] + 1, window[None, :]).astype(f32)
    return window_sum / divisor - as_float[rim_depth:]


def pad_heads(weight, width):
    depth = weight.shape[0]
    heads = weight.shape[1] // width
    shaped = weight.reshape(depth, heads, width)
    return jnp.pad(shaped, ((0, 0), (0, 0), (0, LANES - width))).reshape(depth, heads * LANES)


def pad_row(gain):
    return jnp.pad(gain, (0, LANES - gain.shape[0])).reshape(1, LANES)


def rope_tables(rows, blocks):
    half = ROPE // 2
    frequency = rope_theta ** (-jnp.arange(0, ROPE, 2, dtype=f32) / ROPE)

    def make(positions):
        angles = positions.astype(f32)[:, None] * frequency[None, :]
        cosine, sine = jnp.cos(angles), jnp.sin(angles)
        count = positions.shape[0]
        rest = LANES - HEAD
        cos_row = jnp.concatenate(
            [jnp.ones((count, NOPE), f32), cosine, cosine, jnp.zeros((count, rest), f32)], axis=1
        )
        sin_row = jnp.concatenate(
            [jnp.zeros((count, NOPE), f32), sine, sine, jnp.zeros((count, rest), f32)], axis=1
        )
        return cos_row, sin_row

    return make(jnp.arange(rows)) + make(jnp.arange(blocks) * rows)


def head_finish(x, gain, cosine, sin_low, sin_high):
    factor = lax.rsqrt(jnp.sum(x * x, axis=1, keepdims=True) * (1.0 / HEAD) + norm_eps)
    y = x * factor * gain
    half = ROPE // 2
    return (
        y * cosine
        + pltpu.roll(y, LANES - half, 1) * sin_low
        + pltpu.roll(y, half, 1) * sin_high
    )


def attention_kernel(
    heads,
    step_rows,
    q_ref,
    kv_ref,
    own_ref,
    wq_ref,
    wk_ref,
    wv_ref,
    qlat_gain,
    kvlat_gain,
    qh_gain,
    kh_gain,
    cos_r,
    sin_r,
    cos_b,
    sin_b,
    out_ref,
    kv_buf,
    queries,
    keys_t,
    values,
    acc,
    own_buf,
    sem,
    own_sem,
):
    rows = q_ref.shape[0]
    kvlat = wk_ref.shape[0]
    mine = lax.axis_index("sp")
    lane = lax.broadcasted_iota(jnp.int32, (step_rows, LANES), 1)
    score_scale = HEAD ** (-0.5) * math.log2(math.e)

    def fetch(block, slot):
        return pltpu.make_async_copy(kv_ref.at[block], kv_buf.at[slot], sem.at[slot])

    own_copy = pltpu.make_async_copy(own_ref, own_buf, own_sem)
    own_copy.start()

    @pl.when(mine > 0)
    def _():
        fetch(0, 0).start()

    def angles(block, at):
        cr, sr = cos_r[at, :], sin_r[at, :]
        cb, sb = cos_b[pl.ds(block, 1), :], sin_b[pl.ds(block, 1), :]
        cosine = jnp.where(lane < NOPE, 1.0, cr * cb - sr * sb)
        sine = sr * cb + cr * sb
        low = jnp.where((lane >= NOPE) & (lane < NOPE + ROPE // 2), -sine, 0.0)
        high = jnp.where((lane >= NOPE + ROPE // 2) & (lane < HEAD), sine, 0.0)
        return cosine, low, high

    def prepare_queries(step, _):
        at = pl.ds(pl.multiple_of(step * step_rows, step_rows), step_rows)
        normed = row_norm(q_ref[at, :], qlat_gain[...]).astype(bf16)
        raw = jnp.dot(normed, wq_ref[...], preferred_element_type=f32).astype(bf16).astype(f32)
        tables = angles(mine, at)
        for h in range(heads):
            x = raw[:, h * LANES : (h + 1) * LANES]
            y = head_finish(x, qh_gain[...], *tables)
            queries[h, at, :] = (y * score_scale).astype(bf16)
        return 0

    lax.fori_loop(0, rows // step_rows, prepare_queries, 0)
    acc[...] = jnp.zeros_like(acc)

    def prepare_keys(block, source):
        def one(step, _):
            at = pl.ds(pl.multiple_of(step * step_rows, step_rows), step_rows)
            latent = source[at, :kvlat]
            shared = source[at, kvlat:].astype(f32)
            normed = row_norm(latent, kvlat_gain[...]).astype(bf16)
            plain = jnp.dot(normed, wk_ref[...], preferred_element_type=f32).astype(bf16).astype(f32)
            value = jnp.dot(normed, wv_ref[...], preferred_element_type=f32)
            tables = angles(block, at)
            for h in range(heads):
                x = plain[:, h * LANES : (h + 1) * LANES] + shared
                y = head_finish(x, kh_gain[...], *tables)
                keys_t[h, :, at] = y.T.astype(bf16)
                v = jnp.where(lane == VDIM, 1.0, value[:, h * LANES : (h + 1) * LANES])
                values[h, at, :] = v.astype(bf16)
            return 0

        lax.fori_loop(0, rows // step_rows, one, 0)

    def accumulate(on_diagonal):
        def one(step, _):
            at = pl.ds(pl.multiple_of(step * step_rows, step_rows), step_rows)
            for h in range(heads):
                scores = jnp.dot(queries[h, at, :], keys_t[h], preferred_element_type=f32)
                weights = jnp.exp2(scores)
                if on_diagonal:
                    q_pos = step * step_rows + lax.broadcasted_iota(jnp.int32, scores.shape, 0)
                    k_pos = lax.broadcasted_iota(jnp.int32, scores.shape, 1)
                    weights = jnp.where(k_pos <= q_pos, weights, 0.0)
                acc[h, at, :] += jnp.dot(weights.astype(bf16), values[h], preferred_element_type=f32)
            return 0

        lax.fori_loop(0, rows // step_rows, one, 0)

    def earlier(block, _):
        slot = lax.rem(block, 2)
        fetch(block, slot).wait()

        @pl.when(block + 1 < mine)
        def _():
            fetch(block + 1, 1 - slot).start()

        prepare_keys(block, kv_buf.at[slot])
        accumulate(False)
        return 0

    lax.fori_loop(0, mine, earlier, 0)
    own_copy.wait()
    prepare_keys(mine, own_buf)
    accumulate(True)

    def finish(step, _):
        at = pl.ds(pl.multiple_of(step * step_rows, step_rows), step_rows)
        parts = []
        for h in range(heads):
            a = acc[h, at, :]
            parts.append(a[:, :VDIM] / a[:, VDIM : VDIM + 1])
        out_ref[at, :] = jnp.concatenate(parts, axis=1).astype(bf16)
        return 0

    lax.fori_loop(0, rows // step_rows, finish, 0)


def attention(q_lat, kv_all, kv_own, wq, wk, wv, gains, tables):
    rows = q_lat.shape[0]
    heads = wq.shape[1] // LANES
    step_rows = math.gcd(rows, 256)
    vm = pl.BlockSpec(memory_space=pltpu.VMEM)
    return pl.pallas_call(
        functools.partial(attention_kernel, heads, step_rows),
        out_shape=jax.ShapeDtypeStruct((rows, heads * VDIM), bf16),
        in_specs=[vm, pl.BlockSpec(memory_space=pl.ANY), pl.BlockSpec(memory_space=pl.ANY)] + [vm] * 11,
        out_specs=vm,
        scratch_shapes=[
            pltpu.VMEM((2,) + kv_all.shape[1:], bf16),
            pltpu.VMEM((heads, rows, LANES), bf16),
            pltpu.VMEM((heads, LANES, rows), bf16),
            pltpu.VMEM((heads, rows, LANES), bf16),
            pltpu.VMEM((heads, rows, LANES), f32),
            pltpu.VMEM(kv_own.shape, bf16),
            pltpu.SemaphoreType.DMA((2,)),
            pltpu.SemaphoreType.DMA,
        ],
        compiler_params=pltpu.CompilerParams(vmem_limit_bytes=48 * 1024 * 1024),
    )(q_lat, kv_all, kv_own, wq, wk, wv, *gains, *tables)


MESH = pl.DeviceIdType.MESH


def remote(src, dst, send_sem, recv_sem, target):
    return pltpu.make_async_remote_copy(
        src_ref=src,
        dst_ref=dst,
        send_sem=send_sem,
        recv_sem=recv_sem,
        device_id=target,
        device_id_type=MESH,
    )


def tp_place():
    me = lax.axis_index("tp")
    return me, lax.rem(me, 2), lax.div(me, 2)


def greet_tp(n_tp, me, barrier):
    for step in range(1, n_tp):
        pl.semaphore_signal(
            barrier, inc=1, device_id={"tp": lax.rem(me + step, n_tp)}, device_id_type=MESH
        )


def tp_gather_kernel(n_tp, x_ref, out_ref, local_sem, own_send, far_send, relay_send, recv):
    me, core, chip = tp_place()
    chips = n_tp // 2
    partner = me + 1 - 2 * core
    barrier = pltpu.get_barrier_semaphore()
    greet_tp(n_tp, me, barrier)
    pl.semaphore_wait(barrier, n_tp - 1)
    far = []
    for step in range(1, chips):
        there = 2 * lax.rem(chip + step, chips) + core
        copy = remote(x_ref, out_ref.at[me], far_send.at[step - 1], recv.at[me], {"tp": there})
        copy.start()
        far.append(copy)
    near = remote(x_ref, out_ref.at[me], own_send, recv.at[me], {"tp": partner})
    near.start()
    keep = pltpu.make_async_copy(x_ref, out_ref.at[me], local_sem)
    keep.start()
    relays = []
    for step in range(1, chips):
        source = 2 * lax.rem(chip + chips - step, chips) + core
        remote(x_ref, out_ref.at[source], far_send.at[step - 1], recv.at[source], {"tp": partner}).wait_recv()
        copy = remote(
            out_ref.at[source],
            out_ref.at[source],
            relay_send.at[step - 1],
            recv.at[source],
            {"tp": partner},
        )
        copy.start()
        relays.append(copy)
    for step in range(chips):
        source = 2 * lax.rem(chip + step, chips) + 1 - core
        remote(x_ref, out_ref.at[source], own_send, recv.at[source], {"tp": partner}).wait_recv()
    for copy in far + relays:
        copy.wait_send()
    near.wait_send()
    keep.wait()


def tp_gather(block, identity):
    n_tp = lax.axis_size("tp")
    vm = pl.BlockSpec(memory_space=pltpu.VMEM)
    others = max(1, n_tp // 2 - 1)
    return pl.pallas_call(
        functools.partial(tp_gather_kernel, n_tp),
        out_shape=jax.ShapeDtypeStruct((n_tp,) + block.shape, block.dtype),
        in_specs=[vm],
        out_specs=vm,
        scratch_shapes=[
            pltpu.SemaphoreType.DMA,
            pltpu.SemaphoreType.DMA,
            pltpu.SemaphoreType.DMA((others,)),
            pltpu.SemaphoreType.DMA((others,)),
            pltpu.SemaphoreType.DMA((n_tp,)),
        ],
        compiler_params=pltpu.CompilerParams(collective_id=identity, has_side_effects=True),
    )(block)


def tp_scatter_kernel(
    n_tp, x_ref, out_ref, pair_buf, sum_buf, far_buf, pair_send, pair_recv, far_send, far_recv
):
    me, core, chip = tp_place()
    chips = n_tp // 2
    partner = me + 1 - 2 * core
    rows = out_ref.shape[0]

    def rows_of(place):
        return x_ref.at[pl.ds(pl.multiple_of(place * rows, rows), rows), :]

    barrier = pltpu.get_barrier_semaphore()
    greet_tp(n_tp, me, barrier)
    pl.semaphore_wait(barrier, n_tp - 1)
    pairs = []
    for step in range(1, chips + 1):
        target_chip = lax.rem(chip + step, chips)
        copy = remote(
            rows_of(2 * target_chip + 1 - core),
            pair_buf.at[step - 1],
            pair_send.at[step - 1],
            pair_recv.at[step - 1],
            {"tp": partner},
        )
        copy.start()
        pairs.append(copy)
    far = []
    for step in range(1, chips):
        there = 2 * lax.rem(chip + step, chips) + core
        pairs[step - 1].wait_recv()
        mine = rows_of(there)[...].astype(f32)
        sum_buf[step - 1] = (mine + pair_buf[step - 1].astype(f32)).astype(bf16)
        copy = remote(
            sum_buf.at[step - 1],
            far_buf.at[step - 1],
            far_send.at[step - 1],
            far_recv.at[step - 1],
            {"tp": there},
        )
        copy.start()
        far.append(copy)
    pairs[chips - 1].wait_recv()
    total = rows_of(me)[...].astype(f32) + pair_buf[chips - 1].astype(f32)
    for step in range(1, chips):
        far[step - 1].wait_recv()
        total = total + far_buf[step - 1].astype(f32)
    out_ref[...] = total.astype(bf16)
    for copy in pairs + far:
        copy.wait_send()


def tp_scatter(partial, identity):
    n_tp = lax.axis_size("tp")
    vm = pl.BlockSpec(memory_space=pltpu.VMEM)
    chips = n_tp // 2
    others = max(1, chips - 1)
    rows, width = partial.shape[0] // n_tp, partial.shape[1]
    return pl.pallas_call(
        functools.partial(tp_scatter_kernel, n_tp),
        out_shape=jax.ShapeDtypeStruct((rows, width), bf16),
        in_specs=[vm],
        out_specs=vm,
        scratch_shapes=[
            pltpu.VMEM((chips, rows, width), bf16),
            pltpu.VMEM((others, rows, width), bf16),
            pltpu.VMEM((others, rows, width), bf16),
            pltpu.SemaphoreType.DMA((chips,)),
            pltpu.SemaphoreType.DMA((chips,)),
            pltpu.SemaphoreType.DMA((others,)),
            pltpu.SemaphoreType.DMA((others,)),
        ],
        compiler_params=pltpu.CompilerParams(
            collective_id=identity, has_side_effects=True, vmem_limit_bytes=40 * 1024 * 1024
        ),
    )(partial)


def sp_gather_kernel(
    n_sp, n_tp, x_ref, out_ref, deep_send, side_send, near_send, far_send, relay_send, recv
):
    me, core, chip = tp_place()
    chips = n_tp // 2
    partner = me + 1 - 2 * core
    shard = lax.axis_index("sp")
    deep, side = lax.div(shard, 2), lax.rem(shard, 2)
    last_deep = n_sp // 2 - 1
    rows = x_ref.shape[0] // n_tp
    other = shard + 1 - 2 * side

    def piece(block, place):
        return out_ref.at[block, pl.ds(pl.multiple_of(place * rows, rows), rows), :]

    own = x_ref.at[pl.ds(pl.multiple_of(me * rows, rows), rows), :]

    barrier = pltpu.get_barrier_semaphore()
    greet_tp(n_tp, me, barrier)
    pl.semaphore_signal(barrier, inc=1, device_id={"sp": other}, device_id_type=MESH)

    @pl.when(deep > 0)
    def _():
        pl.semaphore_signal(barrier, inc=1, device_id={"sp": shard - 2}, device_id_type=MESH)

    @pl.when(deep < last_deep)
    def _():
        pl.semaphore_signal(barrier, inc=1, device_id={"sp": shard + 2}, device_id_type=MESH)

    neighbours = jnp.minimum(deep, 1) + jnp.minimum(last_deep - deep, 1)
    pl.semaphore_wait(barrier, n_tp + neighbours)

    def onward(block, source):
        return remote(source, piece(block, me), deep_send.at[block], recv.at[block, me], {"sp": shard + 2})

    def across(block, source):
        return remote(source, piece(block, me), side_send.at[block], recv.at[block, me], {"sp": other})

    def near(block):
        return remote(piece(block, me), piece(block, me), near_send.at[block], recv.at[block, me], {"tp": partner})

    def far(block, step):
        there = 2 * lax.rem(chip + step, chips) + core
        return remote(
            piece(block, me), piece(block, me), far_send.at[block, step - 1], recv.at[block, me], {"tp": there}
        )

    def relay(block, step):
        source = 2 * lax.rem(chip + chips - step, chips) + core
        return remote(
            piece(block, source),
            piece(block, source),
            relay_send.at[block, step - 1],
            recv.at[block, source],
            {"tp": partner},
        )

    def arrived(block, place):
        remote(
            piece(block, place), piece(block, place), near_send.at[block], recv.at[block, place], {"tp": partner}
        ).wait_recv()

    def spread(block):
        for step in range(1, chips):
            far(block, step).start()
        near(block).start()

    def pass_on(block):
        for step in range(1, chips):
            arrived(block, 2 * lax.rem(chip + chips - step, chips) + core)
            relay(block, step).start()

    @pl.when(deep < last_deep)
    def _():
        onward(shard, own).start()

    @pl.when(side == 0)
    def _():
        across(shard, own).start()

    def receive(k, _):
        block = shard - 2 * k
        arrived(block, me)

        @pl.when(deep < last_deep)
        def _():
            onward(block, piece(block, me)).start()

        across(block, piece(block, me)).start()
        spread(block)
        return 0

    def receive_other(k, _):
        block = other - 2 * k
        arrived(block, me)
        spread(block)
        return 0

    first_other = 1 - side

    def step(k, _):
        @pl.when((k > 0) & (k <= deep))
        def _():
            receive(k, 0)

        @pl.when((k >= first_other) & (k <= deep))
        def _():
            receive_other(k, 0)

        before = k - 1

        @pl.when((before > 0) & (before <= deep))
        def _():
            pass_on(shard - 2 * before)

        @pl.when((before >= first_other) & (before <= deep))
        def _():
            pass_on(other - 2 * before)

        return 0

    lax.fori_loop(0, deep + 2, step, 0)

    def drain(block, _):
        for c in range(chips):
            arrived(block, 2 * c + 1 - core)
        for s in range(1, chips):
            far(block, s).wait_send()
            relay(block, s).wait_send()
        near(block).wait_send()
        return 0

    lax.fori_loop(0, shard, drain, 0)

    def drain_sends(k, _):
        block = shard - 2 * k
        source = piece(block, me)

        @pl.when(deep < last_deep)
        def _():
            onward(block, source).wait_send()

        @pl.when((k > 0) | (side == 0))
        def _():
            across(block, source).wait_send()

        return 0

    lax.fori_loop(0, deep + 1, drain_sends, 0)


def sp_gather(block, identity):
    n_sp, n_tp = lax.axis_size("sp"), lax.axis_size("tp")
    others = max(1, n_tp // 2 - 1)
    hbm = pl.BlockSpec(memory_space=pl.ANY)
    return pl.pallas_call(
        functools.partial(sp_gather_kernel, n_sp, n_tp),
        out_shape=jax.ShapeDtypeStruct((n_sp,) + block.shape, block.dtype),
        in_specs=[hbm],
        out_specs=hbm,
        scratch_shapes=[
            pltpu.SemaphoreType.DMA((n_sp,)),
            pltpu.SemaphoreType.DMA((n_sp,)),
            pltpu.SemaphoreType.DMA((n_sp,)),
            pltpu.SemaphoreType.DMA((n_sp, others)),
            pltpu.SemaphoreType.DMA((n_sp, others)),
            pltpu.SemaphoreType.DMA((n_sp, n_tp)),
        ],
        compiler_params=pltpu.CompilerParams(collective_id=identity, has_side_effects=True),
    )(block)


def local(
    activations,
    in_gain,
    w_pool_in,
    pool_gain,
    w_qlat,
    w_kvlat,
    w_krope,
    qlat_gain,
    kvlat_gain,
    w_qup,
    w_kup,
    w_vup,
    qhead_gain,
    khead_gain,
    w_out_pool,
    w_out_attn,
):
    own_input = tp_gather(activations, 0)
    own_input = own_input.reshape(-1, own_input.shape[-1])
    row_count = own_input.shape[0]
    n_sp = lax.axis_size("sp")
    positions = lax.axis_index("sp") * row_count + jnp.arange(row_count, dtype=jnp.int32)
    normed = row_norm(own_input, in_gain).astype(bf16)
    q_part = jnp.dot(normed, w_qlat, preferred_element_type=f32).astype(bf16)
    kv_part = jnp.dot(normed, w_kvlat, preferred_element_type=f32).astype(bf16)
    krope_pad = jnp.pad(w_krope, ((0, 0), (NOPE, LANES - HEAD)))
    rope_key = jnp.dot(normed, krope_pad, preferred_element_type=f32).astype(bf16)
    q_width = q_part.shape[1]
    latents = tp_gather(jnp.concatenate([q_part, kv_part], axis=1), 1)
    q_lat = jnp.concatenate([latents[i, :, :q_width] for i in range(latents.shape[0])], axis=1)
    kv_lat = jnp.concatenate(
        [latents[i, :, q_width:] for i in range(latents.shape[0])] + [rope_key], axis=1
    )
    kv_all = sp_gather(kv_lat, 2)
    pool_in = jnp.dot(normed, w_pool_in, preferred_element_type=f32).astype(bf16)
    prev_rows = from_behind(pool_in[row_count - rim_depth :], "sp", 1)
    extended = jnp.concatenate([prev_rows, pool_in], axis=0)
    channel_start = lax.axis_index("tp") * pool_in.shape[1]
    pool_out = (pool_mix(extended, positions, channel_start) * pool_gain).astype(bf16)
    attended = attention(
        q_lat,
        kv_all,
        kv_lat,
        pad_heads(w_qup, HEAD),
        pad_heads(w_kup, NOPE),
        pad_heads(w_vup, VDIM),
        (qlat_gain.reshape(1, -1), kvlat_gain.reshape(1, -1), pad_row(qhead_gain), pad_row(khead_gain)),
        rope_tables(row_count, n_sp),
    )
    term = jnp.dot(pool_out, w_out_pool, preferred_element_type=f32)
    attn_term = jnp.dot(attended, w_out_attn, preferred_element_type=f32)
    return tp_scatter((term + attn_term).astype(bf16), 3)


def solution(mesh):
    placed = (
        P(("sp", "tp"), None),
        P(),
        P(None, "tp"),
        P("tp"),
        P(None, "tp"),
        P(None, "tp"),
        P(),
        P(),
        P(),
        P(None, "tp"),
        P(None, "tp"),
        P(None, "tp"),
        P(),
        P(),
        P("tp", None),
        P("tp", None),
    )
    return jax.shard_map(
        local, mesh=mesh, in_specs=placed, out_specs=P(("sp", "tp"), None), check_vma=False
    )
```

```python
import functools
import math

import jax
import jax.numpy as jnp
from jax import lax
from jax.experimental import pallas as pl
from jax.experimental.pallas import tpu as pltpu
from jax.sharding import PartitionSpec as P

GROUP = 256
NOPE = 64
ROPE = 32
VDIM = 64
HEAD = NOPE + ROPE
LANES = 128

norm_eps = 1e-06
rope_theta = 10000.0
rim_depth = 15
bf16 = jnp.bfloat16
f32 = jnp.float32


def from_behind(block, axis, distance):
    devices = range(lax.axis_size(axis))
    route = [(i - distance, i) for i in devices if i - distance in devices]
    return lax.ppermute(block, axis, route)


def row_norm(source, norm_gain):
    as_float = source.astype(f32)
    factor = lax.rsqrt(jnp.mean(as_float * as_float, axis=-1, keepdims=True) + norm_eps)
    return as_float * factor * norm_gain


def pool_mix(extended, positions, channel_start):
    row_count = positions.shape[0]
    width = extended.shape[1]
    channel = channel_start + jnp.arange(width, dtype=jnp.int32)
    window = jnp.left_shift(jnp.int32(2), channel // GROUP)
    as_float = extended.astype(f32)
    total = as_float
    window_sum = None
    for level in range(4):
        span = 1 << level
        total = total + jnp.concatenate([jnp.zeros((span, width), f32), total[:-span]], axis=0)
        chosen = total[rim_depth:]
        if window_sum is None:
            window_sum = chosen
        else:
            window_sum = jnp.where(window[None, :] >= 2 * span, chosen, window_sum)
    divisor = jnp.minimum(positions[:, None] + 1, window[None, :]).astype(f32)
    return window_sum / divisor - as_float[rim_depth:]


def pad_heads(weight_ref, padded_ref, width):
    weight = weight_ref[...].astype(f32)
    padded_ref[...] = jnp.zeros_like(padded_ref)
    for h in range(weight.shape[1] // width):
        head = weight[:, h * width : (h + 1) * width]
        padded_ref[:, h * LANES : h * LANES + width] = head.astype(bf16)


def pad_row(gain):
    return jnp.pad(gain, (0, LANES - gain.shape[0])).reshape(1, LANES)


def rope_tables(rows, blocks):
    half = ROPE // 2
    frequency = rope_theta ** (-jnp.arange(0, ROPE, 2, dtype=f32) / ROPE)

    def make(positions):
        angles = positions.astype(f32)[:, None] * frequency[None, :]
        cosine, sine = jnp.cos(angles), jnp.sin(angles)
        count = positions.shape[0]
        rest = LANES - HEAD
        cos_row = jnp.concatenate(
            [jnp.ones((count, NOPE), f32), cosine, cosine, jnp.zeros((count, rest), f32)], axis=1
        )
        sin_row = jnp.concatenate(
            [jnp.zeros((count, NOPE), f32), sine, sine, jnp.zeros((count, rest), f32)], axis=1
        )
        return cos_row, sin_row

    return make(jnp.arange(rows)) + make(jnp.arange(blocks) * rows)


def head_finish(x, gain, cosine, sin_low, sin_high):
    factor = lax.rsqrt(jnp.sum(x * x, axis=1, keepdims=True) * (1.0 / HEAD) + norm_eps)
    y = x * factor * gain
    half = ROPE // 2
    return (
        y * cosine
        + pltpu.roll(y, LANES - half, 1) * sin_low
        + pltpu.roll(y, half, 1) * sin_high
    )


def attention_kernel(
    heads,
    step_rows,
    q_ref,
    kv_ref,
    own_ref,
    wq_raw,
    wk_raw,
    wv_raw,
    qlat_gain,
    kvlat_gain,
    qh_gain,
    kh_gain,
    cos_r,
    sin_r,
    cos_b,
    sin_b,
    out_ref,
    kv_buf,
    queries,
    keys_t,
    values,
    acc,
    own_buf,
    wq_ref,
    wk_ref,
    wv_ref,
    sem,
    own_sem,
):
    rows = q_ref.shape[0]
    kvlat = wk_ref.shape[0]
    mine = lax.axis_index("sp")
    lane = lax.broadcasted_iota(jnp.int32, (step_rows, LANES), 1)
    score_scale = HEAD ** (-0.5) * math.log2(math.e)

    def fetch(block, slot):
        return pltpu.make_async_copy(kv_ref.at[block], kv_buf.at[slot], sem.at[slot])

    own_copy = pltpu.make_async_copy(own_ref, own_buf, own_sem)
    own_copy.start()

    @pl.when(mine > 0)
    def _():
        fetch(0, 0).start()

    pad_heads(wq_raw, wq_ref, HEAD)
    pad_heads(wk_raw, wk_ref, NOPE)
    pad_heads(wv_raw, wv_ref, VDIM)

    def angles(block, at):
        cr, sr = cos_r[at, :], sin_r[at, :]
        cb, sb = cos_b[pl.ds(block, 1), :], sin_b[pl.ds(block, 1), :]
        cosine = jnp.where(lane < NOPE, 1.0, cr * cb - sr * sb)
        sine = sr * cb + cr * sb
        low = jnp.where((lane >= NOPE) & (lane < NOPE + ROPE // 2), -sine, 0.0)
        high = jnp.where((lane >= NOPE + ROPE // 2) & (lane < HEAD), sine, 0.0)
        return cosine, low, high

    def prepare_queries(step, _):
        at = pl.ds(pl.multiple_of(step * step_rows, step_rows), step_rows)
        normed = row_norm(q_ref[at, :], qlat_gain[...]).astype(bf16)
        raw = jnp.dot(normed, wq_ref[...], preferred_element_type=f32).astype(bf16).astype(f32)
        tables = angles(mine, at)
        for h in range(heads):
            x = raw[:, h * LANES : (h + 1) * LANES]
            y = head_finish(x, qh_gain[...], *tables)
            queries[h, at, :] = (y * score_scale).astype(bf16)
        return 0

    lax.fori_loop(0, rows // step_rows, prepare_queries, 0)
    acc[...] = jnp.zeros_like(acc)

    def prepare_keys(block, source):
        def one(step, _):
            at = pl.ds(pl.multiple_of(step * step_rows, step_rows), step_rows)
            latent = source[at, :kvlat]
            shared = source[at, kvlat:].astype(f32)
            normed = row_norm(latent, kvlat_gain[...]).astype(bf16)
            plain = jnp.dot(normed, wk_ref[...], preferred_element_type=f32).astype(bf16).astype(f32)
            value = jnp.dot(normed, wv_ref[...], preferred_element_type=f32)
            tables = angles(block, at)
            for h in range(heads):
                x = plain[:, h * LANES : (h + 1) * LANES] + shared
                y = head_finish(x, kh_gain[...], *tables)
                keys_t[h, :, at] = y.T.astype(bf16)
                v = jnp.where(lane == VDIM, 1.0, value[:, h * LANES : (h + 1) * LANES])
                values[h, at, :] = v.astype(bf16)
            return 0

        lax.fori_loop(0, rows // step_rows, one, 0)

    def accumulate(on_diagonal):
        def one(step, _):
            at = pl.ds(pl.multiple_of(step * step_rows, step_rows), step_rows)
            for h in range(heads):
                scores = jnp.dot(queries[h, at, :], keys_t[h], preferred_element_type=f32)
                weights = jnp.exp2(scores)
                if on_diagonal:
                    q_pos = step * step_rows + lax.broadcasted_iota(jnp.int32, scores.shape, 0)
                    k_pos = lax.broadcasted_iota(jnp.int32, scores.shape, 1)
                    weights = jnp.where(k_pos <= q_pos, weights, 0.0)
                acc[h, at, :] += jnp.dot(weights.astype(bf16), values[h], preferred_element_type=f32)
            return 0

        lax.fori_loop(0, rows // step_rows, one, 0)

    def earlier(block, _):
        slot = lax.rem(block, 2)
        fetch(block, slot).wait()

        @pl.when(block + 1 < mine)
        def _():
            fetch(block + 1, 1 - slot).start()

        prepare_keys(block, kv_buf.at[slot])
        accumulate(False)
        return 0

    lax.fori_loop(0, mine, earlier, 0)
    own_copy.wait()
    prepare_keys(mine, own_buf)
    accumulate(True)

    def finish(step, _):
        at = pl.ds(pl.multiple_of(step * step_rows, step_rows), step_rows)
        parts = []
        for h in range(heads):
            a = acc[h, at, :]
            parts.append(a[:, :VDIM] / a[:, VDIM : VDIM + 1])
        out_ref[at, :] = jnp.concatenate(parts, axis=1).astype(bf16)
        return 0

    lax.fori_loop(0, rows // step_rows, finish, 0)


def attention(q_lat, kv_all, kv_own, wq, wk, wv, gains, tables):
    rows = q_lat.shape[0]
    heads = wq.shape[1] // HEAD
    step_rows = math.gcd(rows, 256)
    vm = pl.BlockSpec(memory_space=pltpu.VMEM)
    return pl.pallas_call(
        functools.partial(attention_kernel, heads, step_rows),
        out_shape=jax.ShapeDtypeStruct((rows, heads * VDIM), bf16),
        in_specs=[vm, pl.BlockSpec(memory_space=pl.ANY), pl.BlockSpec(memory_space=pl.ANY)] + [vm] * 11,
        out_specs=vm,
        scratch_shapes=[
            pltpu.VMEM((2,) + kv_all.shape[1:], bf16),
            pltpu.VMEM((heads, rows, LANES), bf16),
            pltpu.VMEM((heads, LANES, rows), bf16),
            pltpu.VMEM((heads, rows, LANES), bf16),
            pltpu.VMEM((heads, rows, LANES), f32),
            pltpu.VMEM(kv_own.shape, bf16),
            pltpu.VMEM((wq.shape[0], heads * LANES), bf16),
            pltpu.VMEM((wk.shape[0], heads * LANES), bf16),
            pltpu.VMEM((wv.shape[0], heads * LANES), bf16),
            pltpu.SemaphoreType.DMA((2,)),
            pltpu.SemaphoreType.DMA,
        ],
        compiler_params=pltpu.CompilerParams(vmem_limit_bytes=48 * 1024 * 1024),
    )(q_lat, kv_all, kv_own, wq, wk, wv, *gains, *tables)


MESH = pl.DeviceIdType.MESH


def remote(src, dst, send_sem, recv_sem, target):
    return pltpu.make_async_remote_copy(
        src_ref=src,
        dst_ref=dst,
        send_sem=send_sem,
        recv_sem=recv_sem,
        device_id=target,
        device_id_type=MESH,
    )


def tp_place():
    me = lax.axis_index("tp")
    return me, lax.rem(me, 2), lax.div(me, 2)


def greet_tp(n_tp, me, barrier):
    for step in range(1, n_tp):
        pl.semaphore_signal(
            barrier, inc=1, device_id={"tp": lax.rem(me + step, n_tp)}, device_id_type=MESH
        )


def tp_gather_kernel(n_tp, x_ref, out_ref, local_sem, own_send, far_send, relay_send, recv):
    me, core, chip = tp_place()
    chips = n_tp // 2
    partner = me + 1 - 2 * core
    barrier = pltpu.get_barrier_semaphore()
    greet_tp(n_tp, me, barrier)
    pl.semaphore_wait(barrier, n_tp - 1)
    far = []
    for step in range(1, chips):
        there = 2 * lax.rem(chip + step, chips) + core
        copy = remote(x_ref, out_ref.at[me], far_send.at[step - 1], recv.at[me], {"tp": there})
        copy.start()
        far.append(copy)
    near = remote(x_ref, out_ref.at[me], own_send, recv.at[me], {"tp": partner})
    near.start()
    keep = pltpu.make_async_copy(x_ref, out_ref.at[me], local_sem)
    keep.start()
    relays = []
    for step in range(1, chips):
        source = 2 * lax.rem(chip + chips - step, chips) + core
        remote(x_ref, out_ref.at[source], far_send.at[step - 1], recv.at[source], {"tp": partner}).wait_recv()
        copy = remote(
            out_ref.at[source],
            out_ref.at[source],
            relay_send.at[step - 1],
            recv.at[source],
            {"tp": partner},
        )
        copy.start()
        relays.append(copy)
    for step in range(chips):
        source = 2 * lax.rem(chip + step, chips) + 1 - core
        remote(x_ref, out_ref.at[source], own_send, recv.at[source], {"tp": partner}).wait_recv()
    for copy in far + relays:
        copy.wait_send()
    near.wait_send()
    keep.wait()


def tp_gather(block, identity):
    n_tp = lax.axis_size("tp")
    vm = pl.BlockSpec(memory_space=pltpu.VMEM)
    others = max(1, n_tp // 2 - 1)
    return pl.pallas_call(
        functools.partial(tp_gather_kernel, n_tp),
        out_shape=jax.ShapeDtypeStruct((n_tp,) + block.shape, block.dtype),
        in_specs=[vm],
        out_specs=vm,
        scratch_shapes=[
            pltpu.SemaphoreType.DMA,
            pltpu.SemaphoreType.DMA,
            pltpu.SemaphoreType.DMA((others,)),
            pltpu.SemaphoreType.DMA((others,)),
            pltpu.SemaphoreType.DMA((n_tp,)),
        ],
        compiler_params=pltpu.CompilerParams(collective_id=identity, has_side_effects=True),
    )(block)


def tp_scatter_kernel(
    n_tp, x_ref, out_ref, pair_buf, sum_buf, far_buf, pair_send, pair_recv, far_send, far_recv
):
    me, core, chip = tp_place()
    chips = n_tp // 2
    partner = me + 1 - 2 * core
    rows = out_ref.shape[0]

    def rows_of(place):
        return x_ref.at[pl.ds(pl.multiple_of(place * rows, rows), rows), :]

    barrier = pltpu.get_barrier_semaphore()
    greet_tp(n_tp, me, barrier)
    pl.semaphore_wait(barrier, n_tp - 1)
    pairs = []
    for step in range(1, chips + 1):
        target_chip = lax.rem(chip + step, chips)
        copy = remote(
            rows_of(2 * target_chip + 1 - core),
            pair_buf.at[step - 1],
            pair_send.at[step - 1],
            pair_recv.at[step - 1],
            {"tp": partner},
        )
        copy.start()
        pairs.append(copy)
    far = []
    for step in range(1, chips):
        there = 2 * lax.rem(chip + step, chips) + core
        pairs[step - 1].wait_recv()
        mine = rows_of(there)[...].astype(f32)
        sum_buf[step - 1] = (mine + pair_buf[step - 1].astype(f32)).astype(bf16)
        copy = remote(
            sum_buf.at[step - 1],
            far_buf.at[step - 1],
            far_send.at[step - 1],
            far_recv.at[step - 1],
            {"tp": there},
        )
        copy.start()
        far.append(copy)
    pairs[chips - 1].wait_recv()
    total = rows_of(me)[...].astype(f32) + pair_buf[chips - 1].astype(f32)
    for step in range(1, chips):
        far[step - 1].wait_recv()
        total = total + far_buf[step - 1].astype(f32)
    out_ref[...] = total.astype(bf16)
    for copy in pairs + far:
        copy.wait_send()


def tp_scatter(partial, identity):
    n_tp = lax.axis_size("tp")
    vm = pl.BlockSpec(memory_space=pltpu.VMEM)
    chips = n_tp // 2
    others = max(1, chips - 1)
    rows, width = partial.shape[0] // n_tp, partial.shape[1]
    return pl.pallas_call(
        functools.partial(tp_scatter_kernel, n_tp),
        out_shape=jax.ShapeDtypeStruct((rows, width), bf16),
        in_specs=[vm],
        out_specs=vm,
        scratch_shapes=[
            pltpu.VMEM((chips, rows, width), bf16),
            pltpu.VMEM((others, rows, width), bf16),
            pltpu.VMEM((others, rows, width), bf16),
            pltpu.SemaphoreType.DMA((chips,)),
            pltpu.SemaphoreType.DMA((chips,)),
            pltpu.SemaphoreType.DMA((others,)),
            pltpu.SemaphoreType.DMA((others,)),
        ],
        compiler_params=pltpu.CompilerParams(
            collective_id=identity, has_side_effects=True, vmem_limit_bytes=40 * 1024 * 1024
        ),
    )(partial)


def sp_gather_kernel(
    n_sp, n_tp, x_ref, out_ref, deep_send, side_send, near_send, far_send, relay_send, recv
):
    me, core, chip = tp_place()
    chips = n_tp // 2
    partner = me + 1 - 2 * core
    shard = lax.axis_index("sp")
    deep, side = lax.div(shard, 2), lax.rem(shard, 2)
    last_deep = n_sp // 2 - 1
    rows = x_ref.shape[0] // n_tp
    other = shard + 1 - 2 * side

    def piece(block, place):
        return out_ref.at[block, pl.ds(pl.multiple_of(place * rows, rows), rows), :]

    own = x_ref.at[pl.ds(pl.multiple_of(me * rows, rows), rows), :]

    barrier = pltpu.get_barrier_semaphore()
    greet_tp(n_tp, me, barrier)
    pl.semaphore_signal(barrier, inc=1, device_id={"sp": other}, device_id_type=MESH)

    @pl.when(deep > 0)
    def _():
        pl.semaphore_signal(barrier, inc=1, device_id={"sp": shard - 2}, device_id_type=MESH)

    @pl.when(deep < last_deep)
    def _():
        pl.semaphore_signal(barrier, inc=1, device_id={"sp": shard + 2}, device_id_type=MESH)

    neighbours = jnp.minimum(deep, 1) + jnp.minimum(last_deep - deep, 1)
    pl.semaphore_wait(barrier, n_tp + neighbours)

    def onward(block, source):
        return remote(source, piece(block, me), deep_send.at[block], recv.at[block, me], {"sp": shard + 2})

    def across(block, source):
        return remote(source, piece(block, me), side_send.at[block], recv.at[block, me], {"sp": other})

    def near(block):
        return remote(piece(block, me), piece(block, me), near_send.at[block], recv.at[block, me], {"tp": partner})

    def far(block, step):
        there = 2 * lax.rem(chip + step, chips) + core
        return remote(
            piece(block, me), piece(block, me), far_send.at[block, step - 1], recv.at[block, me], {"tp": there}
        )

    def relay(block, step):
        source = 2 * lax.rem(chip + chips - step, chips) + core
        return remote(
            piece(block, source),
            piece(block, source),
            relay_send.at[block, step - 1],
            recv.at[block, source],
            {"tp": partner},
        )

    def arrived(block, place):
        remote(
            piece(block, place), piece(block, place), near_send.at[block], recv.at[block, place], {"tp": partner}
        ).wait_recv()

    def spread(block):
        for step in range(1, chips):
            far(block, step).start()
        near(block).start()

    def pass_on(block):
        for step in range(1, chips):
            arrived(block, 2 * lax.rem(chip + chips - step, chips) + core)
            relay(block, step).start()

    @pl.when(deep < last_deep)
    def _():
        onward(shard, own).start()

    @pl.when(side == 0)
    def _():
        across(shard, own).start()

    def receive(k, _):
        block = shard - 2 * k
        arrived(block, me)

        @pl.when(deep < last_deep)
        def _():
            onward(block, piece(block, me)).start()

        across(block, piece(block, me)).start()
        spread(block)
        return 0

    def receive_other(k, _):
        block = other - 2 * k
        arrived(block, me)
        spread(block)
        return 0

    first_other = 1 - side

    def step(k, _):
        @pl.when((k > 0) & (k <= deep))
        def _():
            receive(k, 0)

        @pl.when((k >= first_other) & (k <= deep))
        def _():
            receive_other(k, 0)

        before = k - 1

        @pl.when((before > 0) & (before <= deep))
        def _():
            pass_on(shard - 2 * before)

        @pl.when((before >= first_other) & (before <= deep))
        def _():
            pass_on(other - 2 * before)

        return 0

    lax.fori_loop(0, deep + 2, step, 0)

    def drain(block, _):
        for c in range(chips):
            arrived(block, 2 * c + 1 - core)
        for s in range(1, chips):
            far(block, s).wait_send()
            relay(block, s).wait_send()
        near(block).wait_send()
        return 0

    lax.fori_loop(0, shard, drain, 0)

    def drain_sends(k, _):
        block = shard - 2 * k
        source = piece(block, me)

        @pl.when(deep < last_deep)
        def _():
            onward(block, source).wait_send()

        @pl.when((k > 0) | (side == 0))
        def _():
            across(block, source).wait_send()

        return 0

    lax.fori_loop(0, deep + 1, drain_sends, 0)


def sp_gather(block, identity):
    n_sp, n_tp = lax.axis_size("sp"), lax.axis_size("tp")
    others = max(1, n_tp // 2 - 1)
    hbm = pl.BlockSpec(memory_space=pl.ANY)
    return pl.pallas_call(
        functools.partial(sp_gather_kernel, n_sp, n_tp),
        out_shape=jax.ShapeDtypeStruct((n_sp,) + block.shape, block.dtype),
        in_specs=[hbm],
        out_specs=hbm,
        scratch_shapes=[
            pltpu.SemaphoreType.DMA((n_sp,)),
            pltpu.SemaphoreType.DMA((n_sp,)),
            pltpu.SemaphoreType.DMA((n_sp,)),
            pltpu.SemaphoreType.DMA((n_sp, others)),
            pltpu.SemaphoreType.DMA((n_sp, others)),
            pltpu.SemaphoreType.DMA((n_sp, n_tp)),
        ],
        compiler_params=pltpu.CompilerParams(collective_id=identity, has_side_effects=True),
    )(block)


def local(
    activations,
    in_gain,
    w_pool_in,
    pool_gain,
    w_qlat,
    w_kvlat,
    w_krope,
    qlat_gain,
    kvlat_gain,
    w_qup,
    w_kup,
    w_vup,
    qhead_gain,
    khead_gain,
    w_out_pool,
    w_out_attn,
):
    own_input = tp_gather(activations, 0)
    own_input = own_input.reshape(-1, own_input.shape[-1])
    row_count = own_input.shape[0]
    n_sp = lax.axis_size("sp")
    positions = lax.axis_index("sp") * row_count + jnp.arange(row_count, dtype=jnp.int32)
    normed = row_norm(own_input, in_gain).astype(bf16)
    q_part = jnp.dot(normed, w_qlat, preferred_element_type=f32).astype(bf16)
    kv_part = jnp.dot(normed, w_kvlat, preferred_element_type=f32).astype(bf16)
    krope_pad = jnp.pad(w_krope, ((0, 0), (NOPE, LANES - HEAD)))
    rope_key = jnp.dot(normed, krope_pad, preferred_element_type=f32).astype(bf16)
    q_width = q_part.shape[1]
    latents = tp_gather(jnp.concatenate([q_part, kv_part], axis=1), 1)
    q_lat = jnp.concatenate([latents[i, :, :q_width] for i in range(latents.shape[0])], axis=1)
    kv_lat = jnp.concatenate(
        [latents[i, :, q_width:] for i in range(latents.shape[0])] + [rope_key], axis=1
    )
    kv_all = sp_gather(kv_lat, 2)
    pool_in = jnp.dot(normed, w_pool_in, preferred_element_type=f32).astype(bf16)
    prev_rows = from_behind(pool_in[row_count - rim_depth :], "sp", 1)
    extended = jnp.concatenate([prev_rows, pool_in], axis=0)
    channel_start = lax.axis_index("tp") * pool_in.shape[1]
    pool_out = (pool_mix(extended, positions, channel_start) * pool_gain).astype(bf16)
    attended = attention(
        q_lat,
        kv_all,
        kv_lat,
        w_qup,
        w_kup,
        w_vup,
        (qlat_gain.reshape(1, -1), kvlat_gain.reshape(1, -1), pad_row(qhead_gain), pad_row(khead_gain)),
        rope_tables(row_count, n_sp),
    )
    term = jnp.dot(pool_out, w_out_pool, preferred_element_type=f32)
    attn_term = jnp.dot(attended, w_out_attn, preferred_element_type=f32)
    return tp_scatter((term + attn_term).astype(bf16), 3)


def solution(mesh):
    placed = (
        P(("sp", "tp"), None),
        P(),
        P(None, "tp"),
        P("tp"),
        P(None, "tp"),
        P(None, "tp"),
        P(),
        P(),
        P(),
        P(None, "tp"),
        P(None, "tp"),
        P(None, "tp"),
        P(),
        P(),
        P("tp", None),
        P("tp", None),
    )
    return jax.shard_map(
        local, mesh=mesh, in_specs=placed, out_specs=P(("sp", "tp"), None), check_vma=False
    )
```
